256 devices in a mesh: ep: 16 (over y, x), tp: 16 (over z, core).
Axes of the slice: x: 4, y: 4, z: 8, core: 2. Of those that a mesh axis runs over, the one named last changes fastest.
Arguments:
- mix_tokens: bfloat16 [32768, 2048], P(('ep', 'tp')), may hold values from -6 to 6
- mix_gain: bfloat16 [2048], replicated, may hold values from 0.099609375 to 1.8984375
- gate_proj: bfloat16 [2048, 1024], P(None, 'tp'), may hold values from -0.125 to 0.125
- conv_proj: bfloat16 [2048, 1024], P(None, 'tp'), may hold values from -0.125 to 0.125
- value_proj: bfloat16 [2048, 1024], P(None, 'tp'), may hold values from -0.125 to 0.125
- conv_taps: bfloat16 [3, 1024], P(None, 'tp'), may hold values from -3 to 3
- out_proj: bfloat16 [1024, 2048], P('tp'), may hold values from -0.1875 to 0.1875
- moe_tokens: bfloat16 [16384, 2048], P(('ep', 'tp')), may hold values from -6 to 6
- moe_gain: bfloat16 [2048], replicated, may hold values from 0.099609375 to 1.8984375
- expert_ids: int32 [16384, 2], P(('ep', 'tp')), may hold values from 0 to 15, all different within a row; in each aligned block of 64 rows (0 to 63, 64 to 127, ...) at most 9 rows name the same one
- expert_scores: float32 [16384, 2], P(('ep', 'tp')), may hold values from -6 to 6
- expert_gate: bfloat16 [16, 2048, 4096], P('ep', None, 'tp'), may hold values from -0.125 to 0.125
- expert_up: bfloat16 [16, 2048, 4096], P('ep', None, 'tp'), may hold values from -0.125 to 0.125
- expert_down: bfloat16 [16, 4096, 2048], P('ep', 'tp'), may hold values from -0.09375 to 0.09375
Outputs:
- mix_out: bfloat16 [32768, 2048], P(('ep', 'tp'))
- moe_out: bfloat16 [16384, 2048], P(('ep', 'tp'))
The draws below stay inside these ranges and needn't reach their ends.
Inputs may be any that keep to these rules, and one draw needn't show every extreme that they name: `expert_ids`: each row names 2 different experts; among the rows of one device no expert is named more than 9 times.
All inputs are finite; a program needn't handle non-finite values.
Results may differ from the reference program's by a relative error of at most 0.018.
Values may be sent and summed in bfloat16 or wider, within the bound.
A program may use at most 128 MiB of HBM per device.

```python
import math
import jax
import jax.numpy as jnp
import numpy as np
from jax import lax

D = 2048
CONV = 1024
FF = 4096
TAPS = 3
TOP = 2
MOE_DEV = 64
EXPERTS = 16
CAP = 9
MIX_TOKENS = 32768
MOE_TOKENS = 16384
N_EP = 16
N_TP = 16


def shard_levels(own_key, dims, shards, low, high):
    gain, own = 1.0, jax.random.fold_in(own_key, 6)
    for dim, blocks in shards:
        draws = jnp.exp(jax.random.uniform(jax.random.fold_in(own, dim), (blocks,), jnp.float32, low / len(shards), high / len(shards)))
        gain = gain * jnp.repeat(draws, dims[dim] // blocks).reshape([-1 if axis == dim else 1 for axis in range(len(dims))])
    return gain


def deal_out(key, own, number, rows, count, top, most, lean):
    order = jax.random.permutation(key, count)
    crowded, ordinary = shares(count, rows * top, most, lean, True), shares(count, rows * top, most, lean, False)
    places = jnp.arange(count)

    def named(tallies, rotation):
        used = int((tallies > 0).sum())
        fixed = max(1, used // 4)
        shifted = fixed + (places - fixed + rotation * (used - fixed)) % max(1, count - fixed)
        return jnp.zeros((count,), jnp.int32).at[order[jnp.where(places < fixed, places, shifted)]].set(jnp.asarray(tallies, jnp.int32))

    tallies = jnp.where(number % 4 == 0, named(crowded, number // 4), named(ordinary, number - number // 4 - 1))
    mixed = jax.random.permutation(jax.random.fold_in(own, 3), count)
    donor, taker = mixed[0:count // 2 * 2:2], mixed[1:count // 2 * 2:2]
    room = jnp.minimum(tallies[donor] - 1, most - tallies[taker]) // 2
    room = jnp.where((donor == order[0]) | (taker == order[0]) | (tallies[taker] == 0), 0, jnp.maximum(room, 0))
    shifted = jax.random.randint(jax.random.fold_in(own, 4), (count // 2,), 0, 1 << 20) % (room + 1)
    tallies = tallies.at[donor].add(-shifted).at[taker].add(shifted)
    labels = jnp.searchsorted(jnp.cumsum(tallies), jnp.arange(rows * top), side="right").astype(jnp.int32)
    listing = labels.reshape(top, rows).T
    listing = listing[jax.random.permutation(jax.random.fold_in(own, 1), rows)]
    rotation = jax.random.randint(jax.random.fold_in(own, 2), (rows, 1), 0, top)
    return jnp.take_along_axis(listing, (jnp.arange(top)[None, :] + rotation) % top, axis=1)


def shares(number_of, total, most, slope, full):
    loads = [(1 << 20) // math.isqrt(standing ** slope) + 1 for standing in range(1, number_of + 1)]
    largest = most if full else min(most, max(-(-total // number_of), total * loads[0] // sum(loads)))
    least = 1 if total - largest >= number_of - 1 else 0
    given, surplus = [largest] + [least] * (number_of - 1), total - largest - least * (number_of - 1)
    while surplus > 0:
        candidates = [i for i in range(1, number_of) if given[i] < largest] or [i for i in range(1, number_of) if given[i] < most]
        mass, budget = sum([loads[i] for i in candidates]), surplus
        for i in candidates:
            addition = min(most - given[i], max(1, budget * loads[i] // mass), surplus)
            given[i] = given[i] + addition
            surplus = surplus - addition
    return np.array(given)


def centred(own_key, extent, spread, reach, split=(), kind=jnp.bfloat16):
    values = jax.random.normal(own_key, extent, jnp.float32) * spread
    if len(split) > 0:
        values = shard_levels(own_key, extent, split, -0.22, 0.18) * values
    return jnp.clip(values, min=-reach, max=reach).astype(kind)


def setup_inputs(seed: int = 0) -> dict:
    keys = jax.random.split(jax.random.key(seed), 15)
    mix_tokens = centred(keys[0], (MIX_TOKENS, D), 1.0, 6.0, ((0, 256),))
    mix_gain = jnp.clip(1.0 + 0.18 * jax.random.normal(keys[1], (D,), jnp.float32), 0.099609375, 1.8984375).astype(jnp.bfloat16)
    gate_proj = centred(keys[2], (D, CONV), D ** -0.5, 0.125, ((1, 16),))
    conv_proj = centred(keys[3], (D, CONV), D ** -0.5, 0.125, ((1, 16),))
    value_proj = centred(keys[4], (D, CONV), D ** -0.5, 0.125, ((1, 16),))
    conv_taps = centred(keys[5], (TAPS, CONV), 0.577, 3.0, ((1, 16),))
    out_proj = centred(keys[6], (CONV, D), CONV ** -0.5, 0.1875, ((0, 16),))
    moe_tokens = centred(keys[7], (MOE_TOKENS, D), 1.0, 6.0, ((0, 256),))
    moe_gain = jnp.clip(1.0 + 0.18 * jax.random.normal(keys[8], (D,), jnp.float32), 0.099609375, 1.8984375).astype(jnp.bfloat16)
    expert_ids_keys = jax.random.split(jax.random.fold_in(keys[9], 1), MOE_TOKENS // MOE_DEV)
    expert_ids_turns = jax.random.permutation(jax.random.fold_in(keys[9], 3), MOE_TOKENS // MOE_DEV)
    expert_ids = jax.vmap(lambda own, number: deal_out(jax.random.fold_in(keys[9], 2), own, number, MOE_DEV, EXPERTS, TOP, CAP, 2))(expert_ids_keys, expert_ids_turns).reshape((MOE_TOKENS, TOP))
    expert_scores = centred(keys[10], (MOE_TOKENS, TOP), 1.0, 6.0, ((0, 256),), jnp.float32)
    expert_gate = centred(keys[11], (EXPERTS, D, FF), D ** -0.5, 0.125, ((0, 16), (2, 16)))
    expert_up = centred(keys[12], (EXPERTS, D, FF), D ** -0.5, 0.125, ((0, 16), (2, 16)))
    expert_down = centred(keys[13], (EXPERTS, FF, D), FF ** -0.5, 0.09375, ((0, 16), (1, 16)))
    return {"mix_tokens": mix_tokens, "mix_gain": mix_gain, "gate_proj": gate_proj, "conv_proj": conv_proj, "value_proj": value_proj, "conv_taps": conv_taps, "out_proj": out_proj, "moe_tokens": moe_tokens, "moe_gain": moe_gain, "expert_ids": expert_ids, "expert_scores": expert_scores, "expert_gate": expert_gate, "expert_up": expert_up, "expert_down": expert_down}


norm_eps = 1e-06

def scaled_norm(row_data, gain_vec):
    values = row_data.astype(jnp.float32)
    inverse = lax.rsqrt(lax.optimization_barrier(jnp.mean(values * values, axis=1, keepdims=True)) + norm_eps)
    return (values * inverse * gain_vec.astype(jnp.float32)).astype(jnp.bfloat16)

def reference(mix_tokens, mix_gain, gate_proj, conv_proj, value_proj, conv_taps, out_proj, moe_tokens, moe_gain, expert_ids, expert_scores, expert_gate, expert_up, expert_down):
    normed = scaled_norm(mix_tokens, mix_gain)
    out_gate = jnp.dot(normed, gate_proj, preferred_element_type=jnp.float32).astype(jnp.bfloat16)
    in_gate = jnp.dot(normed, conv_proj, preferred_element_type=jnp.float32).astype(jnp.bfloat16)
    values = jnp.dot(normed, value_proj, preferred_element_type=jnp.float32).astype(jnp.bfloat16)
    signal = (in_gate.astype(jnp.float32) * values.astype(jnp.float32)).astype(jnp.bfloat16)
    length = signal.shape[0]
    padded = jnp.concatenate([jnp.zeros((TAPS - 1, CONV), jnp.bfloat16), signal], axis=0)
    tap_values = conv_taps.astype(jnp.float32)
    convolved = jnp.zeros((length, CONV), jnp.float32)
    for offset in range(TAPS):
        convolved = convolved + padded[offset:offset + length].astype(jnp.float32) * tap_values[offset]
    carried = (out_gate.astype(jnp.float32) * convolved).astype(jnp.bfloat16)
    mix_out = jnp.dot(carried, out_proj, preferred_element_type=jnp.float32).astype(jnp.bfloat16)
    moe_normed = scaled_norm(moe_tokens, moe_gain)
    flat_ids = expert_ids.reshape(-1).astype(jnp.int32)
    assigned = flat_ids.shape[0]
    bound = N_EP * N_TP * CAP
    onehot = (flat_ids[:, None] == jnp.arange(EXPERTS, dtype=jnp.int32)[None, :]).astype(jnp.int32)
    slot_rank = lax.optimization_barrier(jnp.sum((jnp.cumsum(onehot, axis=0) - onehot) * onehot, axis=1)).astype(jnp.int32)
    owner = (jnp.arange(assigned, dtype=jnp.int32) // TOP).astype(jnp.int32)
    table = jnp.zeros((EXPERTS, bound), jnp.int32).at[flat_ids, slot_rank].set(owner)
    hidden_block = FF // N_TP

    def one_expert(expert_index):
        chosen = moe_normed[table[expert_index]]
        gate_value = jnp.dot(chosen, expert_gate[expert_index], preferred_element_type=jnp.float32)
        up_value = jnp.dot(chosen, expert_up[expert_index], preferred_element_type=jnp.float32)
        hidden = (jax.nn.silu(gate_value) * up_value).astype(jnp.bfloat16)
        down = expert_down[expert_index]

        def add_block(block_index, running):
            start = (block_index * hidden_block).astype(jnp.int32)
            part_hidden = lax.dynamic_slice_in_dim(hidden, start, hidden_block, 1)
            part_weight = lax.dynamic_slice_in_dim(down, start, hidden_block, 0)
            term = jnp.dot(part_hidden, part_weight, preferred_element_type=jnp.float32).astype(jnp.bfloat16)
            term = lax.optimization_barrier(term)
            return running + term.astype(jnp.float32)
        running = lax.fori_loop(0, N_TP, add_block, jnp.zeros((bound, D), jnp.float32))
        return running.astype(jnp.bfloat16)
    results = lax.map(one_expert, jnp.arange(EXPERTS, dtype=jnp.int32))
    picked = results[flat_ids, slot_rank].reshape(-1, TOP, D)
    route_weight = jax.nn.softmax(expert_scores.astype(jnp.float32), axis=1)
    moe_out = lax.optimization_barrier(jnp.sum(route_weight[:, :, None] * picked.astype(jnp.float32), axis=1)).astype(jnp.bfloat16)
    return (mix_out, moe_out)
```

```python
import jax
import jax.numpy as jnp
from jax import lax
from jax.experimental import pallas as pl
from jax.experimental.pallas import tpu as pltpu
from jax.sharding import PartitionSpec as P

norm_eps = 1e-06
MESH = pl.DeviceIdType.MESH
F32 = jnp.float32
BF16 = jnp.bfloat16


def scaled_norm(row_data, gain_vec):
    values = row_data.astype(F32)
    inverse = lax.rsqrt(jnp.mean(values * values, axis=1, keepdims=True) + norm_eps)
    return (values * inverse * gain_vec.astype(F32)).astype(BF16)


def expert_kernel(
    x_ref, wg_ref, wu_ref, wd_ref, out_ref,
    wgp, wup, wdp, ag, ag4, part, part4, own, rs,
    w_send, w_recv, ag_send, ag_recv, rs_send, rs_recv,
):
    ep = lax.axis_index("ep")
    tp = lax.axis_index("tp")
    count = lax.axis_size("tp")
    right = lax.rem(tp + 2, count)
    left = lax.rem(tp + count - 2, count)
    partner = tp + 1 - 2 * lax.rem(tp, 2)
    width = x_ref.shape[1]
    half = width // 2

    barrier = pltpu.get_barrier_semaphore()
    for other in (left, right, partner):
        pl.semaphore_signal(barrier, inc=1, device_id=(ep, other), device_id_type=MESH)
    pl.semaphore_wait(barrier, 3)

    towards = (right, left)

    def copy(src, dst, send, recv, target):
        return pltpu.make_async_remote_copy(
            src_ref=src, dst_ref=dst, send_sem=send, recv_sem=recv,
            device_id=(ep, target), device_id_type=MESH,
        )

    def cols(h):
        return pl.ds(h * half, half)

    gather = {}
    for direction in (0, 1):
        for step in range(1, 5):
            for h in ((0, 1) if step < 4 else (direction,)):
                index = (step - 1) * 2 + (h if step < 4 else 0)
                src = x_ref.at[:, cols(h)] if step == 1 else ag.at[step - 2, direction, :, cols(h)]
                dst = ag.at[step - 1, direction, :, cols(h)] if step < 4 else ag4.at[:, cols(h)]
                gather[direction, step, h] = copy(
                    src, dst, ag_send.at[direction, index], ag_recv.at[direction, index], towards[direction]
                )
    for h in (0, 1):
        for direction in (0, 1):
            gather[direction, 1, h].start()
    weights = [
        copy(wg_ref, wgp, w_send.at[0], w_recv.at[0], partner),
        copy(wu_ref, wup, w_send.at[1], w_recv.at[1], partner),
        copy(wd_ref, wdp, w_send.at[2], w_recv.at[2], partner),
    ]
    for c in weights:
        c.start()

    def ffn(x):
        total = None
        for gate, up, down in ((wg_ref, wu_ref, wd_ref), (wgp, wup, wdp)):
            g = jnp.dot(x, gate[...], preferred_element_type=F32)
            u = jnp.dot(x, up[...], preferred_element_type=F32)
            hidden = (g / (1.0 + jnp.exp(-g)) * u).astype(BF16)
            term = jnp.dot(hidden, down[...], preferred_element_type=F32)
            total = term if total is None else total + term
        return total

    for c in weights:
        c.wait_recv()
    own[...] = ffn(x_ref[...])

    rows = x_ref.shape[0]
    for step in range(1, 4):
        for h in (0, 1):
            for direction in (0, 1):
                gather[direction, step, h].wait_recv()
                if step < 3 or h == direction:
                    gather[direction, step + 1, h].start()
        x = ag[step - 1].reshape(2 * rows, width)
        part[step - 1] = ffn(x).astype(BF16).reshape(2, rows, width)

    scatter = {}
    for direction in (0, 1):
        for step in range(4):
            for h in ((0, 1) if step > 0 else (direction,)):
                index = 0 if step == 0 else step * 2 - 1 + h
                src = part4.at[:, cols(h)] if step == 0 else part.at[3 - step, 1 - direction, :, cols(h)]
                scatter[direction, step, h] = copy(
                    src, rs.at[step, direction, :, cols(h)],
                    rs_send.at[direction, index], rs_recv.at[direction, index], towards[direction],
                )
    for direction in (0, 1):
        scatter[direction, 1, 1 - direction].start()
    for direction in (0, 1):
        gather[direction, 4, direction].wait_recv()
    part4[...] = ffn(ag4[...]).astype(BF16)
    for direction in (0, 1):
        scatter[direction, 0, direction].start()
    for direction in (0, 1):
        h = direction
        scatter[direction, 0, h].wait_recv()
        part[2, 1 - direction, :, cols(h)] = (
            part[2, 1 - direction, :, cols(h)].astype(F32) + rs[0, direction, :, cols(h)].astype(F32)
        ).astype(BF16)
        scatter[direction, 1, h].start()
    for step in (2, 3):
        for order in (0, 1):
            for direction in (0, 1):
                h = (1 - direction) if order == 0 else direction
                scatter[direction, step - 1, h].wait_recv()
                part[3 - step, 1 - direction, :, cols(h)] = (
                    part[3 - step, 1 - direction, :, cols(h)].astype(F32)
                    + rs[step - 1, direction, :, cols(h)].astype(F32)
                ).astype(BF16)
                scatter[direction, step, h].start()
    for h in (0, 1):
        for direction in (0, 1):
            scatter[direction, 3, h].wait_recv()
    out_ref[...] = (own[...] + rs[3, 0].astype(F32) + rs[3, 1].astype(F32)).astype(BF16)
    for c in list(gather.values()) + weights + list(scatter.values()):
        c.wait_send()


def experts_ring(rows, w_gate, w_up, w_down):
    count, width = rows.shape
    hidden = w_gate.shape[1]
    vmem = pl.BlockSpec(memory_space=pltpu.VMEM)
    dma = pltpu.SemaphoreType.DMA
    return pl.pallas_call(
        expert_kernel,
        out_shape=jax.ShapeDtypeStruct((count, width), BF16),
        in_specs=[vmem] * 4,
        out_specs=vmem,
        scratch_shapes=[
            pltpu.VMEM((width, hidden), BF16),
            pltpu.VMEM((width, hidden), BF16),
            pltpu.VMEM((hidden, width), BF16),
            pltpu.VMEM((3, 2, count, width), BF16),
            pltpu.VMEM((count, width), BF16),
            pltpu.VMEM((3, 2, count, width), BF16),
            pltpu.VMEM((count, width), BF16),
            pltpu.VMEM((count, width), F32),
            pltpu.VMEM((4, 2, count, width), BF16),
            dma((3,)), dma((3,)), dma((2, 7)), dma((2, 7)), dma((2, 7)), dma((2, 7)),
        ],
        compiler_params=pltpu.CompilerParams(
            collective_id=0, has_side_effects=True, vmem_limit_bytes=48 * 1024 * 1024
        ),
        cost_estimate=pl.CostEstimate(flops=80_000_000_000, bytes_accessed=4_000_000, transcendentals=0),
    )(rows, w_gate, w_up, w_down)


def shards(
    mix_tokens, mix_gain, gate_proj, conv_proj, value_proj, conv_taps, out_proj,
    moe_tokens, moe_gain, expert_ids, expert_scores, expert_gate, expert_up, expert_down,
):
    n_ep, n_tp = lax.axis_size("ep"), lax.axis_size("tp")
    ep, tp = lax.axis_index("ep"), lax.axis_index("tp")
    core = lax.rem(tp, 2)
    channels = gate_proj.shape[1]
    width = mix_tokens.shape[1]
    same_core = [list(range(0, n_tp, 2)), list(range(1, n_tp, 2))]
    swap = [(t, t ^ 1) for t in range(n_tp)]
    flat = ("ep", "tp")

    joined = jnp.concatenate([gate_proj.T, conv_proj.T, value_proj.T, out_proj], axis=0)
    piece_rows = joined.shape[0] // n_ep
    piece = lax.dynamic_slice_in_dim(joined, ep * piece_rows, piece_rows, 0)
    column = lax.all_gather(piece, "tp", axis=0, tiled=False, axis_index_groups=same_core)
    weights = lax.all_gather(column, "ep", axis=0, tiled=False)
    taps = lax.all_gather(conv_taps, "tp", axis=0, tiled=False, axis_index_groups=same_core)
    per = channels // piece_rows
    taps = taps.reshape(n_tp // 2, 3, per, piece_rows).transpose(1, 2, 0, 3).reshape(3, -1).astype(F32)

    moe_normed = scaled_norm(moe_tokens, moe_gain)
    experts = n_ep
    row_count, top_count = expert_ids.shape
    capacity = top_count * row_count // experts + max(1, top_count * row_count // (8 * experts))
    flat_ids = expert_ids.reshape(-1)
    onehot = (flat_ids[:, None] == jnp.arange(experts, dtype=jnp.int32)[None, :]).astype(jnp.int32)
    slot_rank = jnp.sum((jnp.cumsum(onehot, axis=0) - onehot) * onehot, axis=1)
    slot_index = flat_ids * capacity + slot_rank
    slot_match = slot_index[:, None] == jnp.arange(experts * capacity, dtype=jnp.int32)[None, :]
    dispatch_map = jnp.any(slot_match.reshape(row_count, top_count, experts * capacity), axis=1).astype(BF16)
    outgoing = lax.dot_general(
        dispatch_map, moe_normed, (((0,), (0,)), ((), ())), preferred_element_type=F32
    ).astype(BF16)
    arrived = lax.all_to_all(
        outgoing.reshape(experts, capacity, width), "ep", split_axis=0, concat_axis=0, tiled=True
    )
    summed = experts_ring(arrived.reshape(-1, width), expert_gate[0], expert_up[0], expert_down[0])
    returned = lax.all_to_all(
        summed.reshape(experts, capacity, width), "ep", split_axis=0, concat_axis=0, tiled=True
    )
    picked = returned.reshape(experts * capacity, width)[slot_index].reshape(row_count, top_count, width)
    route_weight = jax.nn.softmax(expert_scores, axis=1)
    moe_out = jnp.sum(route_weight[:, :, None] * picked.astype(F32), axis=1).astype(BF16)

    normed = scaled_norm(mix_tokens, mix_gain)
    total = n_ep * n_tp
    halo = lax.ppermute(normed[-16:], flat, [(i, i + 1) for i in range(total - 1)])
    both = jnp.concatenate([halo, normed], axis=0)
    theirs = lax.ppermute(both, "tp", swap)
    before = jnp.where(core == 0, halo, theirs[:16])
    rows = jnp.concatenate([before, normed, theirs[16:]], axis=0)
    in_rows = weights[: 3 * n_ep // 4].reshape(-1, width)
    combined = lax.dot_general(
        rows, in_rows, (((1,), (1,)), ((), ())), preferred_element_type=F32
    ).astype(BF16)
    wide = combined.shape[1] // 3
    out_gate = combined[:, :wide]
    signal = (combined[:, wide : 2 * wide].astype(F32) * combined[:, 2 * wide :].astype(F32)).astype(BF16).astype(F32)
    count = normed.shape[0]
    sig_halo, sig_own, sig_their = signal[14:16], signal[16 : 16 + count], signal[16 + count :]
    prev_own = jnp.where(core == 0, sig_halo, sig_their[-2:])
    prev_their = jnp.where(core == 0, sig_own[-2:], sig_halo)

    def carry(prev, sig, gate):
        ext = jnp.concatenate([prev, sig], axis=0)
        conv = jnp.zeros((count, wide), F32)
        for k in range(3):
            conv = conv + ext[k : k + count] * taps[k]
        return (gate.astype(F32) * conv).astype(BF16)

    carried = jnp.concatenate(
        [
            carry(prev_own, sig_own, out_gate[16 : 16 + count]),
            carry(prev_their, sig_their, out_gate[16 + count :]),
        ],
        axis=0,
    )
    out_rows = weights[3 * n_ep // 4 :].reshape(-1, width)
    partial = jnp.dot(carried, out_rows, preferred_element_type=F32)
    other = lax.ppermute(partial[count:].astype(BF16), "tp", swap)
    mix_out = (partial[:count] + other.astype(F32)).astype(BF16)
    return (mix_out, moe_out)


def solution(mesh):
    in_specs = (
        P(("ep", "tp"), None), P(), P(None, "tp"), P(None, "tp"), P(None, "tp"), P(None, "tp"), P("tp", None),
        P(("ep", "tp"), None), P(), P(("ep", "tp"), None), P(("ep", "tp"), None),
        P("ep", None, "tp"), P("ep", None, "tp"), P("ep", "tp", None),
    )
    out_specs = (P(("ep", "tp"), None), P(("ep", "tp"), None))
    return jax.shard_map(shards, mesh=mesh, in_specs=in_specs, out_specs=out_specs, check_vma=False)
```
